32 devices in a mesh: sp: 4 (over z), fs: 4 (over y, x), tp: 2 (over core).
Axes of the slice: x: 2, y: 2, z: 4, core: 2. Of those that a mesh axis runs over, the one named last changes fastest.
Arguments:
- tokens: bfloat16 [4, 1024, 1024], P('fs', 'sp', 'tp'), may hold values from -6 to 6
- w_inner: bfloat16 [1024, 2048], P('sp', 'tp'), may hold values from -0.1875 to 0.1875
- w_gate: bfloat16 [1024, 2048], P('sp', 'tp'), may hold values from -0.1875 to 0.1875
- w_write: bfloat16 [1024, 512], P('sp', 'tp'), may hold values from -0.1875 to 0.1875
- w_read: bfloat16 [1024, 512], P('sp', 'tp'), may hold values from -0.1875 to 0.1875
- w_pool_in: bfloat16 [1024, 1024], P('sp', 'tp'), may hold values from -0.1875 to 0.1875
- w_step: bfloat16 [1024, 2, 32], replicated, may hold values from -0.1875 to 0.1875
- conv_inner: bfloat16 [5, 2048], replicated, may hold values from -2.5 to 2.5
- conv_cross: bfloat16 [5, 2, 512], replicated, may hold values from -2.5 to 2.5
- rate_log: float32 [2, 32], replicated, may hold values from -20 to -3
- decay_extra: float32 [4, 1024, 2, 32], P('fs', 'sp', None, 'tp'), may hold values from -1 to 0
- norm_gain: float32 [2048], replicated, may hold values from 0.1 to 1.9
- pool_mix: bfloat16 [4, 256, 256], replicated, may hold values from -0.375 to 0.375
- pool_gain: float32 [1024], replicated, may hold values from 0.1 to 1.9
- w_out_inner: bfloat16 [2048, 1024], P('tp', 'fs'), may hold values from -0.109375 to 0.109375
- w_out_pool: bfloat16 [1024, 1024], P('tp', 'fs'), may hold values from -0.109375 to 0.109375
Outputs:
- layer_out: bfloat16 [4, 1024, 1024], P('fs', ('sp', 'tp'))
The draws below stay inside these ranges and needn't reach their ends.
All inputs are finite; a program needn't handle non-finite values.
Results may differ from the reference program's by a relative error of at most 0.0075.
Values may be sent and summed in bfloat16 or wider, within the bound.
A program may use at most 128 MiB of HBM per device.

```python
import math
import jax
import jax.numpy as jnp
from jax import lax

D = 1024
MIXER_HEADS = 32
HEAD_DIM = 64
GROUPS = 4
STATE = 128
POOL_DIM = 256
POOL_GROUPS = 4
CONV = 5
BLOCK = 128
GRID_W = 32
TOK_DEV = 256
INNER = 2048
POOL = 1024
SEQUENCE_LENGTH = 1024
SEQUENCE_COUNT = 4
N_TP = 2


def draw_rate_log(key, part):
    pick_key, rapid_random_key, gentle_key = jax.random.split(jax.random.fold_in(key, 7), 3)
    fast_share = 0.5
    chosen = jax.random.uniform(pick_key, (2, MIXER_HEADS), jnp.float32) < fast_share
    quick = jax.random.uniform(rapid_random_key, (2, MIXER_HEADS), jnp.float32, math.log(1.0 / 80.0), math.log(1.0 / 25.0))
    gentle = jax.random.uniform(gentle_key, (2, MIXER_HEADS), jnp.float32, math.log(0.05), math.log(0.25)) - math.log(SEQUENCE_LENGTH)
    return jnp.where(chosen, quick, gentle).astype(jnp.float32)


def draw_decay_extra(key, part):
    level_key, position_random_key, depth_random_key, count_random_key = jax.random.split(jax.random.fold_in(key, 13), 4)
    devices_along = SEQUENCE_LENGTH // TOK_DEV
    spike_slot_list = 12
    level_low = 0.05
    level_high = 5.0
    retained_lower = 0.4
    retained_upper = 0.8
    levels = jnp.exp(jax.random.uniform(level_key, (SEQUENCE_COUNT, devices_along, 1, 2, MIXER_HEADS), jnp.float32, math.log(level_low), math.log(level_high)))
    steady_level = jnp.broadcast_to(levels, (SEQUENCE_COUNT, devices_along, TOK_DEV, 2, MIXER_HEADS)).reshape(SEQUENCE_COUNT, SEQUENCE_LENGTH, 2, MIXER_HEADS) * (-1.0 / SEQUENCE_LENGTH)
    spike_positions = jax.random.randint(position_random_key, (SEQUENCE_COUNT, spike_slot_list, 2, MIXER_HEADS), 0, SEQUENCE_LENGTH)
    spike_counts = jax.random.randint(count_random_key, (SEQUENCE_COUNT, 1, 2, MIXER_HEADS), 0, spike_slot_list + 1)
    retained_fraction = jax.random.uniform(depth_random_key, (SEQUENCE_COUNT, spike_slot_list, 2, MIXER_HEADS), jnp.float32, retained_lower, retained_upper)
    slot_ranking = jnp.arange(spike_slot_list, dtype=jnp.int32)[None, :, None, None]
    spike_logarithms = jnp.where(slot_ranking < spike_counts, jnp.log(retained_fraction), 0.0)
    sequence_number = jnp.broadcast_to(jnp.arange(SEQUENCE_COUNT, dtype=jnp.int32)[:, None, None, None], spike_positions.shape)
    direction_number = jnp.broadcast_to(jnp.arange(2, dtype=jnp.int32)[None, None, :, None], spike_positions.shape)
    head_number = jnp.broadcast_to(jnp.arange(MIXER_HEADS, dtype=jnp.int32)[None, None, None, :], spike_positions.shape)
    spike_events = jnp.zeros((SEQUENCE_COUNT, SEQUENCE_LENGTH, 2, MIXER_HEADS), jnp.float32).at[sequence_number, spike_positions, direction_number, head_number].min(spike_logarithms)
    return (steady_level + spike_events).astype(jnp.float32)


def level_of(rng, dims, cuts, least, top_value):
    gain, own = 1.0, jax.random.fold_in(rng, 6)
    for axis_at, parts in cuts:
        heights = jnp.exp(jax.random.uniform(jax.random.fold_in(own, axis_at), (parts,), jnp.float32, least / len(cuts), top_value / len(cuts)))
        gain = gain * jnp.repeat(heights, dims[axis_at] // parts).reshape([-1 if axis == axis_at else 1 for axis in range(len(dims))])
    return gain


def gaussian(own_key, shape, spread, reach, cuts=(), kind=jnp.bfloat16):
    level = level_of(own_key, shape, cuts, -0.22, 0.18) if cuts else 1.0
    values = jax.random.normal(own_key, shape, jnp.float32) * spread * level
    return jnp.minimum(jnp.maximum(values, -reach), reach).astype(kind)


def setup_inputs(seed: int = 0) -> dict:
    streams_of = jax.random.split(jax.random.key(seed), 17)
    tokens = gaussian(streams_of[0], (SEQUENCE_COUNT, SEQUENCE_LENGTH, D), 1.0, 6.0, ((0, 4), (1, 4), (2, 2)))
    w_inner = gaussian(streams_of[1], (D, INNER), D ** -0.5, 0.1875, ((0, 4), (1, 2)))
    w_gate = gaussian(streams_of[2], (D, INNER), D ** -0.5, 0.1875, ((0, 4), (1, 2)))
    w_write = gaussian(streams_of[3], (D, GROUPS * STATE), D ** -0.5, 0.1875, ((0, 4), (1, 2)))
    w_read = gaussian(streams_of[4], (D, GROUPS * STATE), D ** -0.5, 0.1875, ((0, 4), (1, 2)))
    w_pool_in = gaussian(streams_of[5], (D, POOL), D ** -0.5, 0.1875, ((0, 4), (1, 2)))
    w_step = gaussian(streams_of[6], (D, 2, MIXER_HEADS), D ** -0.5, 0.1875)
    conv_inner = gaussian(streams_of[7], (CONV, INNER), CONV ** -0.5, 2.5)
    conv_cross = gaussian(streams_of[8], (CONV, 2, GROUPS * STATE), CONV ** -0.5, 2.5)
    rate_log = draw_rate_log(jax.random.fold_in(streams_of[16], 71), 0)
    decay_extra = draw_decay_extra(jax.random.fold_in(streams_of[16], 71), 0)
    norm_gain = jnp.clip(1.0 + 0.18 * jax.random.normal(streams_of[11], (INNER,), jnp.float32), 0.1, 1.9)
    pool_mix = gaussian(streams_of[12], (POOL_GROUPS, POOL_DIM, POOL_DIM), POOL_DIM ** -0.5, 0.375)
    pool_gain = jnp.clip(1.0 + 0.18 * jax.random.normal(streams_of[13], (POOL,), jnp.float32), 0.1, 1.9)
    w_out_inner = gaussian(streams_of[14], (INNER, D), (MIXER_HEADS * HEAD_DIM + POOL_GROUPS * POOL_DIM) ** -0.5, 0.109375, ((0, 2), (1, 4)))
    w_out_pool = gaussian(streams_of[15], (POOL, D), (MIXER_HEADS * HEAD_DIM + POOL_GROUPS * POOL_DIM) ** -0.5, 0.109375, ((0, 2), (1, 4)))
    return {"tokens": tokens, "w_inner": w_inner, "w_gate": w_gate, "w_write": w_write, "w_read": w_read, "w_pool_in": w_pool_in, "w_step": w_step, "conv_inner": conv_inner, "conv_cross": conv_cross, "rate_log": rate_log, "decay_extra": decay_extra, "norm_gain": norm_gain, "pool_mix": pool_mix, "pool_gain": pool_gain, "w_out_inner": w_out_inner, "w_out_pool": w_out_pool}


HIGHEST = lax.Precision.HIGHEST
EPSILON = 1e-05

def centred_taps(streams, conv_taps):
    half_width = conv_taps.shape[0] // 2
    length = streams.shape[0]
    padded = jnp.pad(streams, ((half_width, half_width), (0, 0)))
    running = jnp.zeros_like(streams)
    for offset in range(conv_taps.shape[0]):
        running = running + padded[offset:offset + length] * conv_taps[offset]
    return running

def state_pass(values, decays, writer_rows, read_rows):
    length = decays.shape[0]
    blocks = length // BLOCK
    per_group = MIXER_HEADS // GROUPS
    lower_mask = jnp.tril(jnp.ones((BLOCK, BLOCK), dtype=bool))[:, :, None]

    def to_blocks(array):
        return array.reshape((blocks, BLOCK) + array.shape[1:])

    def advance(carried, pieces):
        block_values, block_decays, block_writes, block_reads = pieces
        cumulative = jnp.cumsum(block_decays, axis=0)
        segment_log = cumulative[:, None, :] - cumulative[None, :, :]
        weights = jnp.exp(jnp.where(lower_mask, segment_log, -jnp.inf))
        scores = jnp.einsum('ign,jgn->ijg', block_reads, block_writes, precision=HIGHEST)
        scores = jnp.repeat(scores, per_group, axis=2)
        inside = jnp.einsum('ijh,jhp->ihp', scores * weights, block_values, precision=HIGHEST)
        reads_head = jnp.repeat(block_reads, per_group, axis=1)
        carried_out = jnp.einsum('ihn,hpn->ihp', reads_head, carried, precision=HIGHEST) * jnp.exp(cumulative)[:, :, None]
        tail_decay = jnp.exp(cumulative[-1:] - cumulative)
        writes_head = jnp.repeat(block_writes, per_group, axis=1)
        fresh = jnp.einsum('jhn,jhp->hpn', writes_head * tail_decay[:, :, None], block_values, precision=HIGHEST)
        carried = carried * jnp.exp(cumulative[-1])[:, None, None] + fresh
        return (carried, inside + carried_out)
    zero_state = jnp.zeros((MIXER_HEADS, HEAD_DIM, STATE), jnp.float32)
    last_state, outputs = lax.scan(advance, zero_state, (to_blocks(values), to_blocks(decays), to_blocks(writer_rows), to_blocks(read_rows)))
    return outputs.reshape(length, MIXER_HEADS, HEAD_DIM)

def window_sum(values, mesh_direction, window):
    extent = values.shape[mesh_direction]
    widths = [(0, 0)] * values.ndim
    widths[mesh_direction] = (1, 0)
    running = jnp.cumsum(jnp.pad(values, widths), axis=mesh_direction)
    places = jnp.arange(extent).astype(jnp.int32)
    lower_end = jnp.clip(places - window // 2, 0, extent).astype(jnp.int32)
    upper_end = jnp.clip(places - window // 2 + window, 0, extent).astype(jnp.int32)
    summed = jnp.take(running, upper_end, axis=mesh_direction) - jnp.take(running, lower_end, axis=mesh_direction)
    return (summed, (upper_end - lower_end).astype(jnp.float32))

def pool_mixer(pool_in, pool_mix, pool_gain):
    grid_rows = pool_in.shape[0] // GRID_W
    grid = pool_in.astype(jnp.float32).reshape(grid_rows, GRID_W, POOL_GROUPS, POOL_DIM)
    results = []
    for group_index in range(POOL_GROUPS):
        window = 2 ** (group_index + 1)
        channel_plane = grid[:, :, group_index]
        summed, row_counts = window_sum(channel_plane, 0, window)
        summed, col_counts = window_sum(summed, 1, window)
        average = summed / (row_counts[:, None, None] * col_counts[None, :, None])
        offsets = (average - channel_plane).astype(jnp.bfloat16).reshape(-1, POOL_DIM)
        mixed_rows = jnp.dot(offsets, pool_mix[group_index], preferred_element_type=jnp.float32)
        gain_part = pool_gain[group_index * POOL_DIM:(group_index + 1) * POOL_DIM]
        results.append((mixed_rows * gain_part).astype(jnp.bfloat16))
    return jnp.concatenate(results, axis=1)

def one_sequence(tokens, decay_extra, weights):
    w_inner, w_gate, w_write, w_read, w_pool_in, w_step, conv_inner, conv_cross, rate_log, norm_gain, pool_mix, pool_gain, w_out_inner, w_out_pool = weights
    length = tokens.shape[0]
    cross_width = GROUPS * STATE
    inner_x = jnp.dot(tokens, w_inner, preferred_element_type=jnp.float32).astype(jnp.bfloat16)
    gate_in = jnp.dot(tokens, w_gate, preferred_element_type=jnp.float32).astype(jnp.bfloat16)
    write_in = jnp.dot(tokens, w_write, preferred_element_type=jnp.float32).astype(jnp.bfloat16)
    read_in = jnp.dot(tokens, w_read, preferred_element_type=jnp.float32).astype(jnp.bfloat16)
    pool_in = jnp.dot(tokens, w_pool_in, preferred_element_type=jnp.float32).astype(jnp.bfloat16)
    raw_step = jnp.dot(tokens, w_step.reshape(D, 2 * MIXER_HEADS), preferred_element_type=jnp.float32).reshape(length, 2, MIXER_HEADS)
    streams = jnp.concatenate([inner_x, write_in, read_in], axis=1).astype(jnp.float32)
    conv_taps = jnp.concatenate([conv_inner, conv_cross[:, 0], conv_cross[:, 1]], axis=1).astype(jnp.float32)
    activated = jax.nn.silu(centred_taps(streams, conv_taps))
    values = activated[:, :INNER].reshape(length, MIXER_HEADS, HEAD_DIM)
    writer_rows = activated[:, INNER:INNER + cross_width].reshape(length, GROUPS, STATE)
    read_rows = activated[:, INNER + cross_width:].reshape(length, GROUPS, STATE)
    step_size = jax.nn.softplus(raw_step)
    log_decay = -step_size * jnp.exp(rate_log)[None] + decay_extra
    forward = state_pass(values * step_size[:, 0, :, None], log_decay[:, 0], writer_rows, read_rows)
    backward = state_pass((values * step_size[:, 1, :, None])[::-1], log_decay[::-1, 1], writer_rows[::-1], read_rows[::-1])[::-1]
    gated_out = (forward + backward) * jax.nn.silu(gate_in.astype(jnp.float32)).reshape(length, MIXER_HEADS, HEAD_DIM)
    rms_scale = lax.rsqrt(lax.optimization_barrier(jnp.mean(gated_out * gated_out, axis=2, keepdims=True)) + EPSILON)
    mixer_out = (gated_out * rms_scale * norm_gain.reshape(MIXER_HEADS, HEAD_DIM)).reshape(length, INNER).astype(jnp.bfloat16)
    pooled = pool_mixer(pool_in, pool_mix, pool_gain)
    inner_part = INNER // N_TP
    pool_part = POOL // N_TP
    summed = jnp.zeros((length, D), jnp.float32)
    for tp_rank in range(N_TP):
        inner_cols = slice(tp_rank * inner_part, (tp_rank + 1) * inner_part)
        pool_cols = slice(tp_rank * pool_part, (tp_rank + 1) * pool_part)
        partial_value = jnp.dot(mixer_out[:, inner_cols], w_out_inner[inner_cols], preferred_element_type=jnp.float32)
        partial_value = partial_value + jnp.dot(pooled[:, pool_cols], w_out_pool[pool_cols], preferred_element_type=jnp.float32)
        rounded = lax.optimization_barrier(partial_value.astype(jnp.bfloat16))
        summed = summed + rounded.astype(jnp.float32)
    return summed.astype(jnp.bfloat16)

def reference(tokens, w_inner, w_gate, w_write, w_read, w_pool_in, w_step, conv_inner, conv_cross, rate_log, decay_extra, norm_gain, pool_mix, pool_gain, w_out_inner, w_out_pool):
    weights = (w_inner, w_gate, w_write, w_read, w_pool_in, w_step, conv_inner, conv_cross, rate_log, norm_gain, pool_mix, pool_gain, w_out_inner, w_out_pool)

    def run_sequence(sequence_pair):
        return one_sequence(sequence_pair[0], sequence_pair[1], weights)
    return lax.map(run_sequence, (tokens, decay_extra))
```

```python
import functools

import jax
import jax.numpy as jnp
from jax import lax
from jax.experimental import pallas as pl
from jax.experimental.pallas import tpu as pltpu
from jax.sharding import PartitionSpec as P

HEAD_DIM = 64
STATE = 128
POOL_DIM = 256
POOL_GROUPS = 4
CONV = 5
GRID_W = 32
EPSILON = 1e-05
HIGHEST = lax.Precision.HIGHEST
MESH = pl.DeviceIdType.MESH
RIM = 16
NH = 2

bf16 = jnp.bfloat16
f32 = jnp.float32


def dot(a, b, precision=None):
    return jnp.dot(a, b, preferred_element_type=f32, precision=precision)


def remote(src, dst, send, recv, axis, target):
    return pltpu.make_async_remote_copy(
        src_ref=src,
        dst_ref=dst,
        send_sem=send,
        recv_sem=recv,
        device_id={axis: target},
        device_id_type=MESH,
    )


def greet(sizes):
    barrier = pltpu.get_barrier_semaphore()
    n_s, n_f, n_t = sizes
    count = 0
    for axis, steps, n in (
        ("sp", (1, n_s - 1), n_s),
        ("fs", range(1, n_f), n_f),
        ("tp", range(1, n_t), n_t),
    ):
        me = lax.axis_index(axis)
        for j in steps:
            pl.semaphore_signal(
                barrier, inc=1, device_id={axis: lax.rem(me + j, n)}, device_id_type=MESH
            )
            count += 1
    pl.semaphore_wait(barrier, count)


def project_kernel(
    sizes, tok, w_inner, w_write, w_read, w_gate, w_pool, w_step,
    out, raw, rim_lo, rim_hi, pool_lo, pool_hi,
    stacked, wg, tg, pbuf,
    up_send, up_recv, dn_send, dn_recv, ft_send, ft_recv, tt_send, tt_recv,
    a_send, a_recv, h_send, h_recv,
):
    n_s, n_f, n_t = sizes
    s, f, t = lax.axis_index("sp"), lax.axis_index("fs"), lax.axis_index("tp")
    rows, half_d = tok.shape
    ks, total = stacked.shape
    share = total // n_f
    hw = share // NH
    stream = rim_lo.shape[1]

    at = 0
    for ref in (w_inner, w_write, w_read, w_gate, w_pool):
        stacked[:, at : at + ref.shape[1]] = ref[...]
        at += ref.shape[1]
    tg[f, t] = tok[...]
    greet(sizes)

    def weight_copy(hh, c, up):
        piece = wg.at[hh, pl.ds(pl.multiple_of(c * ks, ks), ks)]
        if up:
            return remote(piece, piece, up_send.at[hh, c], up_recv.at[hh, c], "sp", s + 1)
        return remote(piece, piece, dn_send.at[hh, c], dn_recv.at[hh, c], "sp", s - 1)

    def column(who, hh):
        return pl.ds(pl.multiple_of(who * share + hh * hw, 128), hw)

    for hh in range(NH):
        wg[hh, pl.ds(pl.multiple_of(s * ks, ks), ks)] = stacked[:, column(f, hh)]

    def relay(hh, k):
        for up in (True, False):
            c = s - k if up else s + k
            inside = c >= 0 if up else c < n_s
            more = s + 1 < n_s if up else s >= 1

            @pl.when(inside)
            def _():
                if k > 0:
                    weight_copy(hh, c, up).wait_recv()

                @pl.when(more)
                def _():
                    weight_copy(hh, c, up).start()

    def tok_fs(j):
        return remote(
            tg.at[f, t], tg.at[f, t], ft_send.at[j], ft_recv.at[j], "fs", lax.rem(f + j, n_f)
        )

    def tok_fs_in(j):
        who = lax.rem(f + n_f - j, n_f)
        return remote(tg.at[who, t], tg.at[who, t], ft_send.at[j], ft_recv.at[j], "fs", who)

    def tok_tp(j, i):
        who = lax.rem(f + n_f - j, n_f)
        to = lax.rem(t + i, n_t)
        return remote(tg.at[who, t], tg.at[who, t], tt_send.at[j, i], tt_recv.at[j, i], "tp", to)

    def tok_tp_in(j, i):
        who = lax.rem(f + n_f - j, n_f)
        src = lax.rem(t + n_t - i, n_t)
        return remote(
            tg.at[who, src], tg.at[who, src], tt_send.at[j, i], tt_recv.at[j, i], "tp", src
        )

    relay(0, 0)
    for j in range(1, n_f):
        tok_fs(j).start()
    for i in range(1, n_t):
        tok_tp(0, i).start()
    for k in range(1, n_s):
        if k == n_s - 1:
            for j in range(1, n_f):
                tok_fs_in(j).wait_recv()
                for i in range(1, n_t):
                    tok_tp(j, i).start()
        relay(0, k)

    def product(who, hh):
        acc = dot(tg[who, 0], wg[hh, 0:half_d])
        for i in range(1, n_t):
            acc = acc + dot(tg[who, i], wg[hh, i * half_d : (i + 1) * half_d])
        return acc.astype(bf16)

    def answer(hh, j):
        return remote(
            pbuf.at[hh, j - 1],
            out.at[:, column(f, hh)],
            a_send.at[hh, j - 1],
            a_recv.at[hh, j - 1],
            "fs",
            lax.rem(f + j, n_f),
        )

    def answer_in(hh, j):
        who = lax.rem(f + n_f - j, n_f)
        return remote(
            pbuf.at[hh, j - 1],
            out.at[:, column(who, hh)],
            a_send.at[hh, j - 1],
            a_recv.at[hh, j - 1],
            "fs",
            who,
        )

    for hh in range(NH):
        if hh + 1 < NH:
            relay(hh + 1, 0)
        if hh == 0:
            for j in range(n_f):
                for i in range(1, n_t):
                    tok_tp_in(j, i).wait_recv()
        for j in range(1, n_f):
            pbuf[hh, j - 1] = product(lax.rem(f + j, n_f), hh)
            answer(hh, j).start()
        out[:, column(f, hh)] = product(f, hh)
        if hh == 0:
            step = dot(tg[f, 0], w_step[0:half_d])
            for i in range(1, n_t):
                step = step + dot(tg[f, i], w_step[i * half_d : (i + 1) * half_d])
            raw[...] = step
        if hh + 1 < NH:
            for k in range(1, n_s):
                relay(hh + 1, k)

    for hh in range(NH):
        for j in range(1, n_f):
            answer_in(hh, j).wait_recv()

    pool_at = total - pool_lo.shape[1]
    halo = (
        (out.at[rows - RIM : rows, 0:stream], rim_lo, 0, True),
        (out.at[:, pool_at:total], pool_lo, 1, True),
        (out.at[0:RIM, 0:stream], rim_hi, 2, False),
        (out.at[:, pool_at:total], pool_hi, 3, False),
    )

    def halo_copy(item):
        src, dst, sem, up = item
        return remote(src, dst, h_send.at[sem], h_recv.at[sem], "sp", s + 1 if up else s - 1)

    for item in halo:
        up = item[3]

        @pl.when(s + 1 < n_s if up else s >= 1)
        def _():
            halo_copy(item).start()

        @pl.when(s == 0 if up else s == n_s - 1)
        def _():
            item[1][...] = jnp.zeros_like(item[1])

    for hh in range(NH):
        for k in range(n_s):
            for up in (True, False):
                c = s - k if up else s + k

                @pl.when(
                    jnp.logical_and(c >= 0, s + 1 < n_s)
                    if up
                    else jnp.logical_and(c < n_s, s >= 1)
                )
                def _():
                    weight_copy(hh, c, up).wait_send()

        for j in range(1, n_f):
            answer(hh, j).wait_send()
    for j in range(n_f):
        if j > 0:
            tok_fs(j).wait_send()
        for i in range(1, n_t):
            tok_tp(j, i).wait_send()
    for item in halo:
        up = item[3]

        @pl.when(s >= 1 if up else s + 1 < n_s)
        def _():
            halo_copy(item).wait_recv()

        @pl.when(s + 1 < n_s if up else s >= 1)
        def _():
            halo_copy(item).wait_send()


def mixer_kernel(
    sizes, proj, raw, rim_lo, rim_hi, pool_lo, pool_hi, extra, rate_log, taps, norm_gain,
    mix, pool_gain, wo_inner, wo_pool,
    result,
    frame, act, inside, wo_i, wo_p, sum_f, sum_b, out_f, out_b, in_f, in_b, part, peer, pooled,
    o_send, o_recv, f_send, f_recv, b_send, b_recv, t_send, t_recv,
):
    n_s, n_f, n_t = sizes
    s, f, t = lax.axis_index("sp"), lax.axis_index("fs"), lax.axis_index("tp")
    rows = proj.shape[0]
    stream = rim_lo.shape[1]
    inner = norm_gain.shape[1]
    heads = inner // HEAD_DIM
    cross = (stream - inner) // 2
    groups = cross // STATE
    per = heads // groups
    wide = per * HEAD_DIM
    greet(sizes)

    def out_copy(j, who, n):
        src, dst = ((wo_inner, wo_i), (wo_pool, wo_p))[n]
        return remote(
            src, dst.at[who], o_send.at[j, n], o_recv.at[j, n], "fs", lax.rem(f + j, n_f)
        )

    for j in range(1, n_f):
        for n in range(2):
            out_copy(j, f, n).start()
    wo_i[f] = wo_inner[...]
    wo_p[f] = wo_pool[...]

    step = jax.nn.softplus(raw[...])
    decay = extra[...] - step * jnp.exp(rate_log[...])
    row_id = lax.broadcasted_iota(jnp.int32, (rows, rows), 0)
    col_id = lax.broadcasted_iota(jnp.int32, (rows, rows), 1)
    lower = (row_id >= col_id).astype(f32)
    upper = (row_id <= col_id).astype(f32)
    run_f = dot(lower, decay[:, :heads], HIGHEST)
    run_b = dot(upper, decay[:, heads:], HIGHEST)
    last_f, last_b = run_f[rows - 1 : rows], run_b[0:1]
    spread_r = lax.broadcasted_iota(jnp.int32, (2 * heads, inner), 0)
    spread_c = lax.broadcasted_iota(jnp.int32, (2 * heads, inner), 1)
    spread_m = (lax.rem(spread_r, heads) == spread_c // HEAD_DIM).astype(bf16)
    gather_r = lax.broadcasted_iota(jnp.int32, (inner, heads), 0)
    gather_c = lax.broadcasted_iota(jnp.int32, (inner, heads), 1)
    gather_m = (gather_r // HEAD_DIM == gather_c).astype(bf16)

    def split(x):
        high = x.astype(bf16)
        return high, (x - high.astype(f32)).astype(bf16)

    def spread(x):
        return dot(jnp.concatenate(split(x), axis=1), spread_m)

    frame[0:8] = rim_lo[RIM - 8 : RIM].astype(f32)
    frame[8 : 8 + rows] = proj[:, :stream].astype(f32)
    frame[8 + rows : 16 + rows] = rim_hi[0:8].astype(f32)
    first = 8 - CONV // 2
    total = frame[first : first + rows] * taps[0:1]
    for k in range(1, CONV):
        total = total + frame[first + k : first + k + rows] * taps[k : k + 1]
    act[...] = (total * jax.nn.sigmoid(total)).astype(bf16)

    def cut(kind, g):
        at = inner + kind * cross + g * STATE
        return act[:, at : at + STATE]

    tail_f = spread(jnp.exp(last_f - run_f) * step[:, :heads])
    tail_b = spread(jnp.exp(last_b - run_b) * step[:, heads:])
    ones = jnp.ones((8, 1), f32)
    keep_f = spread(jnp.exp(last_f) * ones)[0:1]
    keep_b = spread(jnp.exp(last_b) * ones)[0:1]

    def chain_copy(forward, g):
        src, dst, send, recv = (
            (out_f, in_f, f_send, f_recv) if forward else (out_b, in_b, b_send, b_recv)
        )
        return remote(
            src.at[g], dst.at[g], send.at[g], recv.at[g], "sp", s + 1 if forward else s - 1
        )

    for g in range(groups):
        cols = slice(g * wide, (g + 1) * wide)
        vals = act[:, cols].astype(f32)
        writes = cut(0, g).T
        sum_f[g] = dot(writes, (vals * tail_f[:, cols]).astype(bf16))
        sum_b[g] = dot(writes, (vals * tail_b[:, cols]).astype(bf16))

        @pl.when(s == 0)
        def _():
            in_f[g] = jnp.zeros_like(in_f[g])
            out_f[g] = sum_f[g].astype(bf16)
            chain_copy(True, g).start()

        @pl.when(s == n_s - 1)
        def _():
            in_b[g] = jnp.zeros_like(in_b[g])
            out_b[g] = sum_b[g].astype(bf16)
            chain_copy(False, g).start()

    def hand_on(d):
        @pl.when(s == d)
        def _():
            for g in range(groups):
                chain_copy(True, g).wait_recv()
                if d < n_s - 1:
                    cols = slice(g * wide, (g + 1) * wide)
                    out_f[g] = (in_f[g].astype(f32) * keep_f[:, cols] + sum_f[g]).astype(bf16)
                    chain_copy(True, g).start()

        @pl.when(s == n_s - 1 - d)
        def _():
            for g in range(groups):
                chain_copy(False, g).wait_recv()
                if d < n_s - 1:
                    cols = slice(g * wide, (g + 1) * wide)
                    out_b[g] = (in_b[g].astype(f32) * keep_b[:, cols] + sum_b[g]).astype(bf16)
                    chain_copy(False, g).start()

    after = row_id > col_id
    same = row_id == col_id
    side = jnp.concatenate([run_f, run_b, step], axis=1).T

    def head_part(g):
        def work():
            scores = lax.dot_general(
                cut(1, g), cut(0, g), (((1,), (1,)), ((), ())), preferred_element_type=f32
            )
            for h in range(g * per, (g + 1) * per, 2):
                pair = []
                for a in (h, h + 1):
                    fwd = run_f[:, a : a + 1] - side[a : a + 1]
                    bwd = run_b[:, a : a + 1] - side[heads + a : heads + a + 1]
                    dt_f = side[2 * heads + a : 2 * heads + a + 1]
                    dt_b = side[3 * heads + a : 3 * heads + a + 1]
                    scale = jnp.where(after, dt_f, dt_b) + jnp.where(same, dt_f, 0.0)
                    weight = scores * jnp.exp(jnp.where(after, fwd, bwd)) * scale
                    value = act[:, a * HEAD_DIM : (a + 1) * HEAD_DIM]
                    pair.append(dot(weight.astype(bf16), value))
                inside[:, h * HEAD_DIM : (h + 2) * HEAD_DIM] = jnp.concatenate(pair, axis=1)

        return work

    def pool_part():
        grid_rows = rows // GRID_W
        pool_at = proj.shape[1] - pooled.shape[1]
        here = pooled.shape[1] // POOL_DIM
        r, c = row_id // GRID_W, lax.rem(row_id, GRID_W)
        rj, cj = col_id // GRID_W, lax.rem(col_id, GRID_W)
        one = lax.broadcasted_iota(jnp.int32, (rows, 1), 0)
        r1, c1 = one // GRID_W + s * grid_rows, lax.rem(one, GRID_W)
        for slot in range(here):
            reach = jnp.left_shift(jnp.int32(1), t * here + slot)
            cols = slice(slot * POOL_DIM, (slot + 1) * POOL_DIM)
            col_in = jnp.logical_and(cj - c >= -reach, cj - c < reach)
            box = jnp.zeros((rows, POOL_DIM), f32)
            own = proj[:, pool_at + slot * POOL_DIM : pool_at + (slot + 1) * POOL_DIM]
            for shift, source in (
                (-grid_rows, pool_lo[:, cols]),
                (0, own),
                (grid_rows, pool_hi[:, cols]),
            ):
                gap = rj + shift - r
                mask = jnp.logical_and(jnp.logical_and(gap >= -reach, gap < reach), col_in)
                box = box + dot(mask.astype(f32).astype(bf16), source)
            high_r = jnp.minimum(r1 + reach, n_s * grid_rows)
            n_rows = high_r - jnp.maximum(r1 - reach, 0)
            n_cols = jnp.minimum(c1 + reach, GRID_W) - jnp.maximum(c1 - reach, 0)
            average = box / (n_rows * n_cols).astype(f32)
            offsets = (average - own.astype(f32)).astype(bf16)
            pooled[:, cols] = (dot(offsets, mix[slot]) * pool_gain[:, cols]).astype(bf16)

    works = [head_part(g) for g in range(groups)] + [pool_part]
    for d in range(1, n_s):
        if works:
            works.pop(0)()
        hand_on(d)
    while works:
        works.pop(0)()

    lead_f, lead_b = spread(jnp.exp(run_f)), spread(jnp.exp(run_b))
    for g in range(groups):
        cols = slice(g * wide, (g + 1) * wide)
        reads = cut(1, g)
        mixed = inside[:, cols] + dot(reads, in_f[g]) * lead_f[:, cols]
        mixed = mixed + dot(reads, in_b[g]) * lead_b[:, cols]
        gate = proj[:, stream + g * wide : stream + (g + 1) * wide].astype(f32)
        inside[:, cols] = mixed * (gate * jax.nn.sigmoid(gate))
    gated = inside[...]
    high, low = split(gated * gated)
    mean = (dot(high, gather_m) + dot(low, gather_m)) * (1.0 / HEAD_DIM)
    scale = spread(lax.rsqrt(mean + EPSILON))
    mixer = (gated * scale * norm_gain[...]).astype(bf16)

    for j in range(1, n_f):
        for n in range(2):
            out_copy(j, lax.rem(f + n_f - j, n_f), n).wait_recv()
    width = wo_inner.shape[1]
    for w in range(n_f):
        part[:, w * width : (w + 1) * width] = (
            dot(mixer, wo_i[w]) + dot(pooled[...], wo_p[w])
        ).astype(bf16)

    keep = rows // n_t

    def part_of(who):
        return pl.ds(pl.multiple_of(who * keep, keep), keep)

    def last_copy(i):
        to = lax.rem(t + i, n_t)
        return remote(
            part.at[part_of(to)], peer.at[i - 1], t_send.at[i - 1], t_recv.at[i - 1], "tp", to
        )

    for i in range(1, n_t):
        last_copy(i).start()
    for j in range(1, n_f):
        for n in range(2):
            out_copy(j, f, n).wait_send()
    for g in range(groups):

        @pl.when(s + 1 < n_s)
        def _():
            chain_copy(True, g).wait_send()

        @pl.when(s >= 1)
        def _():
            chain_copy(False, g).wait_send()

    acc = part[part_of(t)].astype(f32)
    for i in range(1, n_t):
        last_copy(i).wait_recv()
        acc = acc + peer[i - 1].astype(f32)
    result[...] = acc.astype(bf16)
    for i in range(1, n_t):
        last_copy(i).wait_send()


def body(
    sizes, tokens, w_inner, w_gate, w_write, w_read, w_pool_in, w_step, conv_inner, conv_cross,
    rate_log, decay_extra, norm_gain, pool_mix, pool_gain, w_out_inner, w_out_pool,
):
    n_s, n_f, n_t = sizes
    tp_rank = lax.axis_index("tp")
    tok = tokens[0]
    rows, half_d = tok.shape
    ks, inner = w_inner.shape
    cross = w_write.shape[1]
    pool = w_pool_in.shape[1]
    heads = inner // HEAD_DIM
    groups = cross // STATE
    stream = inner + 2 * cross
    total = stream + inner + pool
    hw = total // n_f // NH
    d = half_d * n_t

    def mine(array, axis):
        size = array.shape[axis] // n_t
        return lax.dynamic_slice_in_dim(array, tp_rank * size, size, axis)

    step_w = mine(w_step, 2).reshape(d, 2 * heads)
    taps = jnp.concatenate(
        [mine(conv_inner, 1), mine(conv_cross[:, 0], 1), mine(conv_cross[:, 1], 1)], axis=1
    ).astype(f32)
    vmem = pl.BlockSpec(memory_space=pltpu.VMEM)
    dma = pltpu.SemaphoreType.DMA

    def shape(*dims, kind=bf16):
        return jax.ShapeDtypeStruct(dims, kind)

    moved = pl.pallas_call(
        functools.partial(project_kernel, sizes),
        out_shape=(
            shape(rows, total),
            shape(rows, 2 * heads, kind=f32),
            shape(RIM, stream),
            shape(RIM, stream),
            shape(rows, pool),
            shape(rows, pool),
        ),
        in_specs=[vmem] * 7,
        out_specs=(vmem,) * 6,
        scratch_shapes=[
            pltpu.VMEM((ks, total), bf16),
            pltpu.VMEM((NH, d, hw), bf16),
            pltpu.VMEM((n_f, n_t, rows, half_d), bf16),
            pltpu.VMEM((NH, n_f - 1, rows, hw), bf16),
            dma((NH, n_s)), dma((NH, n_s)), dma((NH, n_s)), dma((NH, n_s)),
            dma((n_f,)), dma((n_f,)), dma((n_f, n_t)), dma((n_f, n_t)),
            dma((NH, n_f - 1)), dma((NH, n_f - 1)), dma((4,)), dma((4,)),
        ],
        compiler_params=pltpu.CompilerParams(collective_id=0, has_side_effects=True),
    )(tok, w_inner, w_write, w_read, w_gate, w_pool_in, step_w)

    result = pl.pallas_call(
        functools.partial(mixer_kernel, sizes),
        out_shape=shape(rows // n_t, d),
        in_specs=[vmem] * 14,
        out_specs=vmem,
        scratch_shapes=[
            pltpu.VMEM((rows + 16, stream), f32),
            pltpu.VMEM((rows, stream), bf16),
            pltpu.VMEM((rows, inner), f32),
            pltpu.VMEM((n_f,) + w_out_inner.shape, bf16),
            pltpu.VMEM((n_f,) + w_out_pool.shape, bf16),
            pltpu.VMEM((groups, STATE, inner // groups), f32),
            pltpu.VMEM((groups, STATE, inner // groups), f32),
            pltpu.VMEM((groups, STATE, inner // groups), bf16),
            pltpu.VMEM((groups, STATE, inner // groups), bf16),
            pltpu.VMEM((groups, STATE, inner // groups), bf16),
            pltpu.VMEM((groups, STATE, inner // groups), bf16),
            pltpu.VMEM((rows, d), bf16),
            pltpu.VMEM((n_t - 1, rows // n_t, d), bf16),
            pltpu.VMEM((rows, pool), bf16),
            dma((n_f, 2)), dma((n_f, 2)), dma((groups,)), dma((groups,)),
            dma((groups,)), dma((groups,)), dma((n_t - 1,)), dma((n_t - 1,)),
        ],
        compiler_params=pltpu.CompilerParams(collective_id=1, has_side_effects=True),
    )(
        *moved,
        decay_extra[0].reshape(rows, 2 * heads),
        mine(rate_log, 1).reshape(1, 2 * heads),
        taps,
        mine(norm_gain, 0)[None],
        mine(pool_mix, 0),
        mine(pool_gain, 0)[None],
        w_out_inner,
        w_out_pool,
    )
    return result[None]


def solution(mesh):
    sizes = tuple(mesh.shape[axis] for axis in ("sp", "fs", "tp"))
    return jax.shard_map(
        functools.partial(body, sizes),
        mesh=mesh,
        in_specs=(
            P("fs", "sp", "tp"),
            P("sp", "tp"),
            P("sp", "tp"),
            P("sp", "tp"),
            P("sp", "tp"),
            P("sp", "tp"),
            P(),
            P(),
            P(),
            P(),
            P("fs", "sp", None, "tp"),
            P(),
            P(),
            P(),
            P("tp", "fs"),
            P("tp", "fs"),
        ),
        out_specs=P("fs", ("sp", "tp"), None),
        check_vma=False,
    )
```

```python
import functools

import jax
import jax.numpy as jnp
from jax import lax
from jax.experimental import pallas as pl
from jax.experimental.pallas import tpu as pltpu
from jax.sharding import PartitionSpec as P

HEAD_DIM = 64
STATE = 128
POOL_DIM = 256
POOL_GROUPS = 4
CONV = 5
GRID_W = 32
EPSILON = 1e-05
HIGHEST = lax.Precision.HIGHEST
MESH = pl.DeviceIdType.MESH
RIM = 16
NH = 2

bf16 = jnp.bfloat16
f32 = jnp.float32


def dot(a, b, precision=None):
    return jnp.dot(a, b, preferred_element_type=f32, precision=precision)


def remote(src, dst, send, recv, axis, target):
    return pltpu.make_async_remote_copy(
        src_ref=src,
        dst_ref=dst,
        send_sem=send,
        recv_sem=recv,
        device_id={axis: target},
        device_id_type=MESH,
    )


def pick(array, t, n_t, size, at):
    mine = array[:, at : at + size]
    for i in range(1, n_t):
        mine = jnp.where(t == i, array[:, at + i * size : at + (i + 1) * size], mine)
    return mine


def greet(sizes):
    barrier = pltpu.get_barrier_semaphore()
    n_s, n_f, n_t = sizes
    count = 0
    for axis, steps, n in (
        ("sp", (1, n_s - 1), n_s),
        ("fs", range(1, n_f), n_f),
        ("tp", range(1, n_t), n_t),
    ):
        me = lax.axis_index(axis)
        for j in steps:
            pl.semaphore_signal(
                barrier, inc=1, device_id={axis: lax.rem(me + j, n)}, device_id_type=MESH
            )
            count += 1
    pl.semaphore_wait(barrier, count)


def project_kernel(
    sizes, tok, w_inner, w_write, w_read, w_gate, w_pool, w_step, wo_pool,
    out, raw, rim_lo, rim_hi, pool_lo, pool_hi, wo_p,
    stacked, wg, tg, pbuf,
    up_send, up_recv, dn_send, dn_recv, ft_send, ft_recv, tt_send, tt_recv,
    a_send, a_recv, h_send, h_recv, o_send, o_recv,
):
    n_s, n_f, n_t = sizes
    s, f, t = lax.axis_index("sp"), lax.axis_index("fs"), lax.axis_index("tp")
    rows, half_d = tok.shape
    ks, total = stacked.shape
    share = total // n_f
    hw = share // NH
    stream = rim_lo.shape[1]
    pool_half = (pool_lo.shape[1] - 1) // (n_f * hw)

    at = 0
    for ref in (w_pool, w_gate, w_inner, w_write, w_read):
        stacked[:, at : at + ref.shape[1]] = ref[...]
        at += ref.shape[1]
    tg[f, t] = tok[...]
    greet(sizes)

    def weight_copy(hh, c, up):
        piece = wg.at[hh, pl.ds(pl.multiple_of(c * ks, ks), ks)]
        if up:
            return remote(piece, piece, up_send.at[hh, c], up_recv.at[hh, c], "sp", s + 1)
        return remote(piece, piece, dn_send.at[hh, c], dn_recv.at[hh, c], "sp", s - 1)

    def column(who, hh):
        return pl.ds(pl.multiple_of((hh * n_f + who) * hw, 128), hw)

    for hh in range(NH):
        wg[hh, pl.ds(pl.multiple_of(s * ks, ks), ks)] = stacked[:, column(f, hh)]

    def relay(hh, k):
        for up in (True, False):
            c = s - k if up else s + k
            inside = c >= 0 if up else c < n_s
            more = s + 1 < n_s if up else s >= 1

            @pl.when(inside)
            def _():
                if k > 0:
                    weight_copy(hh, c, up).wait_recv()

                @pl.when(more)
                def _():
                    weight_copy(hh, c, up).start()

    def tok_fs(j):
        return remote(
            tg.at[f, t], tg.at[f, t], ft_send.at[j], ft_recv.at[j], "fs", lax.rem(f + j, n_f)
        )

    def tok_fs_in(j):
        who = lax.rem(f + n_f - j, n_f)
        return remote(tg.at[who, t], tg.at[who, t], ft_send.at[j], ft_recv.at[j], "fs", who)

    def tok_tp(j, i):
        who = lax.rem(f + n_f - j, n_f)
        to = lax.rem(t + i, n_t)
        return remote(tg.at[who, t], tg.at[who, t], tt_send.at[j, i], tt_recv.at[j, i], "tp", to)

    def tok_tp_in(j, i):
        who = lax.rem(f + n_f - j, n_f)
        src = lax.rem(t + n_t - i, n_t)
        return remote(
            tg.at[who, src], tg.at[who, src], tt_send.at[j, i], tt_recv.at[j, i], "tp", src
        )

    def out_copy(j, who):
        to = lax.rem(f + j, n_f)
        return remote(wo_pool, wo_p.at[who], o_send.at[j], o_recv.at[j], "fs", to)

    relay(0, 0)
    for j in range(1, n_f):
        tok_fs(j).start()
    for j in range(1, n_f):
        out_copy(j, f).start()
    for i in range(1, n_t):
        tok_tp(0, i).start()
    wo_p[f] = wo_pool[...]
    for k in range(1, n_s):
        if k == n_s - 1:
            for j in range(1, n_f):
                tok_fs_in(j).wait_recv()
                for i in range(1, n_t):
                    tok_tp(j, i).start()
        relay(0, k)

    def product(who, hh):
        acc = dot(tg[who, 0], wg[hh, 0:half_d])
        for i in range(1, n_t):
            acc = acc + dot(tg[who, i], wg[hh, i * half_d : (i + 1) * half_d])
        return acc.astype(bf16)

    def answer(hh, j):
        return remote(
            pbuf.at[hh, j - 1],
            out.at[:, column(f, hh)],
            a_send.at[hh, j - 1],
            a_recv.at[hh, j - 1],
            "fs",
            lax.rem(f + j, n_f),
        )

    def answer_in(hh, j):
        who = lax.rem(f + n_f - j, n_f)
        return remote(
            pbuf.at[hh, j - 1],
            out.at[:, column(who, hh)],
            a_send.at[hh, j - 1],
            a_recv.at[hh, j - 1],
            "fs",
            who,
        )

    for hh in range(NH):
        if hh + 1 < NH:
            relay(hh + 1, 0)
        if hh == 0:
            for j in range(n_f):
                for i in range(1, n_t):
                    tok_tp_in(j, i).wait_recv()
        for j in range(1, n_f):
            pbuf[hh, j - 1] = product(lax.rem(f + j, n_f), hh)
            answer(hh, j).start()
        out[:, column(f, hh)] = product(f, hh)
        if hh == 0:
            step = dot(tg[f, 0], w_step[0:half_d])
            for i in range(1, n_t):
                step = step + dot(tg[f, i], w_step[i * half_d : (i + 1) * half_d])
            heads = raw.shape[1] // 2
            raw[:, :heads] = pick(step, t, n_t, heads, 0)
            raw[:, heads:] = pick(step, t, n_t, heads, heads * n_t)
        if hh + 1 < NH:
            for k in range(1, n_s):
                relay(hh + 1, k)

    pool = pool_lo.shape[1]
    stream_at = total - stream
    halo = (
        (out.at[:, 0:pool], pool_lo, 0, True),
        (out.at[:, 0:pool], pool_hi, 1, False),
        (out.at[rows - RIM : rows, stream_at:total], rim_lo, 2, True),
        (out.at[0:RIM, stream_at:total], rim_hi, 3, False),
    )

    def halo_copy(item):
        src, dst, sem, up = item
        return remote(src, dst, h_send.at[sem], h_recv.at[sem], "sp", s + 1 if up else s - 1)

    def start_halo(items):
        for item in items:
            up = item[3]

            @pl.when(s + 1 < n_s if up else s >= 1)
            def _():
                halo_copy(item).start()

            @pl.when(s == 0 if up else s == n_s - 1)
            def _():
                item[1][...] = jnp.zeros_like(item[1])

    for hh in range(NH):
        for j in range(1, n_f):
            answer_in(hh, j).wait_recv()
        if hh == pool_half:
            start_halo(halo[:2])
    start_halo(halo[2:])

    for hh in range(NH):
        for k in range(n_s):
            for up in (True, False):
                c = s - k if up else s + k

                @pl.when(
                    jnp.logical_and(c >= 0, s + 1 < n_s)
                    if up
                    else jnp.logical_and(c < n_s, s >= 1)
                )
                def _():
                    weight_copy(hh, c, up).wait_send()

        for j in range(1, n_f):
            answer(hh, j).wait_send()
    for j in range(n_f):
        if j > 0:
            tok_fs(j).wait_send()
            out_copy(j, f).wait_send()
            out_copy(j, lax.rem(f + n_f - j, n_f)).wait_recv()
        for i in range(1, n_t):
            tok_tp(j, i).wait_send()
    for item in halo:
        up = item[3]

        @pl.when(s >= 1 if up else s + 1 < n_s)
        def _():
            halo_copy(item).wait_recv()

        @pl.when(s + 1 < n_s if up else s >= 1)
        def _():
            halo_copy(item).wait_send()


def mixer_kernel(
    sizes, proj, raw, rim_lo, rim_hi, pool_lo, pool_hi, wo_p, extra, rate_log, conv_inner,
    conv_cross, norm_gain, mix, pool_gain, wo_inner,
    result,
    frame, act, inside, wo_i, sum_f, sum_b, out_f, out_b, in_f, in_b, part, peer, pooled,
    o_send, o_recv, f_send, f_recv, b_send, b_recv, t_send, t_recv,
):
    n_s, n_f, n_t = sizes
    s, f, t = lax.axis_index("sp"), lax.axis_index("fs"), lax.axis_index("tp")
    rows = proj.shape[0]
    stream = rim_lo.shape[1]
    inner = norm_gain.shape[1] // n_t
    stream_at = proj.shape[1] - stream
    gate_at = stream_at - inner
    heads = inner // HEAD_DIM
    cross = (stream - inner) // 2
    groups = cross // STATE
    per = heads // groups
    wide = per * HEAD_DIM
    greet(sizes)

    def out_copy(j, who):
        to = lax.rem(f + j, n_f)
        return remote(wo_inner, wo_i.at[who], o_send.at[j], o_recv.at[j], "fs", to)

    for j in range(1, n_f):
        out_copy(j, f).start()
    wo_i[f] = wo_inner[...]

    def own(ref, size, at=0):
        return ref[:, pl.ds(pl.multiple_of(at + t * size, 128), size)].astype(f32)

    step = jax.nn.softplus(raw[...])
    rates = jnp.exp(rate_log[...])
    rates = [pick(rates[k : k + 1], t, n_t, heads, 0) for k in (0, 1)]
    decay = extra[...] - step * jnp.concatenate(rates, axis=1)
    row_id = lax.broadcasted_iota(jnp.int32, (rows, rows), 0)
    col_id = lax.broadcasted_iota(jnp.int32, (rows, rows), 1)
    lower = (row_id >= col_id).astype(f32)
    upper = (row_id <= col_id).astype(f32)
    run_f = dot(lower, decay[:, :heads], HIGHEST)
    run_b = dot(upper, decay[:, heads:], HIGHEST)
    last_f, last_b = run_f[rows - 1 : rows], run_b[0:1]
    spread_r = lax.broadcasted_iota(jnp.int32, (2 * heads, inner), 0)
    spread_c = lax.broadcasted_iota(jnp.int32, (2 * heads, inner), 1)
    spread_m = (lax.rem(spread_r, heads) == spread_c // HEAD_DIM).astype(bf16)
    gather_r = lax.broadcasted_iota(jnp.int32, (inner, heads), 0)
    gather_c = lax.broadcasted_iota(jnp.int32, (inner, heads), 1)
    gather_m = (gather_r // HEAD_DIM == gather_c).astype(bf16)

    def split(x):
        high = x.astype(bf16)
        return high, (x - high.astype(f32)).astype(bf16)

    def spread(x):
        return dot(jnp.concatenate(split(x), axis=1), spread_m)

    frame[0:8] = rim_lo[RIM - 8 : RIM].astype(f32)
    frame[8 : 8 + rows] = proj[:, stream_at:].astype(f32)
    frame[8 + rows : 16 + rows] = rim_hi[0:8].astype(f32)
    taps = jnp.concatenate(
        [own(conv_inner, inner), own(conv_cross, cross), own(conv_cross, cross, cross * n_t)],
        axis=1,
    )
    first = 8 - CONV // 2
    total = frame[first : first + rows] * taps[0:1]
    for k in range(1, CONV):
        total = total + frame[first + k : first + k + rows] * taps[k : k + 1]
    act[...] = (total * jax.nn.sigmoid(total)).astype(bf16)

    def cut(kind, g):
        at = inner + kind * cross + g * STATE
        return act[:, at : at + STATE]

    tail_f = spread(jnp.exp(last_f - run_f) * step[:, :heads])
    tail_b = spread(jnp.exp(last_b - run_b) * step[:, heads:])
    ones = jnp.ones((8, 1), f32)
    keep_f = spread(jnp.exp(last_f) * ones)[0:1]
    keep_b = spread(jnp.exp(last_b) * ones)[0:1]

    def chain_copy(forward, g):
        src, dst, send, recv = (
            (out_f, in_f, f_send, f_recv) if forward else (out_b, in_b, b_send, b_recv)
        )
        return remote(
            src.at[g], dst.at[g], send.at[g], recv.at[g], "sp", s + 1 if forward else s - 1
        )

    for g in range(groups):
        cols = slice(g * wide, (g + 1) * wide)
        vals = act[:, cols].astype(f32)
        writes = cut(0, g).T
        sum_f[g] = dot(writes, (vals * tail_f[:, cols]).astype(bf16))
        sum_b[g] = dot(writes, (vals * tail_b[:, cols]).astype(bf16))

        @pl.when(s == 0)
        def _():
            in_f[g] = jnp.zeros_like(in_f[g])
            out_f[g] = sum_f[g].astype(bf16)
            chain_copy(True, g).start()

        @pl.when(s == n_s - 1)
        def _():
            in_b[g] = jnp.zeros_like(in_b[g])
            out_b[g] = sum_b[g].astype(bf16)
            chain_copy(False, g).start()

    def hand_on(d):
        @pl.when(s == d)
        def _():
            for g in range(groups):
                chain_copy(True, g).wait_recv()
                if d < n_s - 1:
                    cols = slice(g * wide, (g + 1) * wide)
                    out_f[g] = (in_f[g].astype(f32) * keep_f[:, cols] + sum_f[g]).astype(bf16)
                    chain_copy(True, g).start()

        @pl.when(s == n_s - 1 - d)
        def _():
            for g in range(groups):
                chain_copy(False, g).wait_recv()
                if d < n_s - 1:
                    cols = slice(g * wide, (g + 1) * wide)
                    out_b[g] = (in_b[g].astype(f32) * keep_b[:, cols] + sum_b[g]).astype(bf16)
                    chain_copy(False, g).start()

    after = row_id > col_id
    same = row_id == col_id
    side = jnp.concatenate([run_f, run_b, step], axis=1).T

    def head_part(g):
        def work():
            scores = lax.dot_general(
                cut(1, g), cut(0, g), (((1,), (1,)), ((), ())), preferred_element_type=f32
            )
            for h in range(g * per, (g + 1) * per, 2):
                pair = []
                for a in (h, h + 1):
                    fwd = run_f[:, a : a + 1] - side[a : a + 1]
                    bwd = run_b[:, a : a + 1] - side[heads + a : heads + a + 1]
                    dt_f = side[2 * heads + a : 2 * heads + a + 1]
                    dt_b = side[3 * heads + a : 3 * heads + a + 1]
                    scale = jnp.where(after, dt_f, dt_b) + jnp.where(same, dt_f, 0.0)
                    weight = scores * jnp.exp(jnp.where(after, fwd, bwd)) * scale
                    value = act[:, a * HEAD_DIM : (a + 1) * HEAD_DIM]
                    pair.append(dot(weight.astype(bf16), value))
                inside[:, h * HEAD_DIM : (h + 2) * HEAD_DIM] = jnp.concatenate(pair, axis=1)

        return work

    def pool_part():
        grid_rows = rows // GRID_W
        gains = own(pool_gain, pooled.shape[1])
        here = pooled.shape[1] // POOL_DIM
        r, c = row_id // GRID_W, lax.rem(row_id, GRID_W)
        rj, cj = col_id // GRID_W, lax.rem(col_id, GRID_W)
        one = lax.broadcasted_iota(jnp.int32, (rows, 1), 0)
        r1, c1 = one // GRID_W + s * grid_rows, lax.rem(one, GRID_W)
        for slot in range(here):
            reach = jnp.left_shift(jnp.int32(1), t * here + slot)
            cols = slice(slot * POOL_DIM, (slot + 1) * POOL_DIM)
            col_in = jnp.logical_and(cj - c >= -reach, cj - c < reach)
            box = jnp.zeros((rows, POOL_DIM), f32)
            centre = proj[:, cols]
            for shift, source in (
                (-grid_rows, pool_lo[:, cols]),
                (0, centre),
                (grid_rows, pool_hi[:, cols]),
            ):
                gap = rj + shift - r
                mask = jnp.logical_and(jnp.logical_and(gap >= -reach, gap < reach), col_in)
                box = box + dot(mask.astype(f32).astype(bf16), source)
            high_r = jnp.minimum(r1 + reach, n_s * grid_rows)
            n_rows = high_r - jnp.maximum(r1 - reach, 0)
            n_cols = jnp.minimum(c1 + reach, GRID_W) - jnp.maximum(c1 - reach, 0)
            average = box / (n_rows * n_cols).astype(f32)
            offsets = (average - centre.astype(f32)).astype(bf16)
            pooled[:, cols] = (dot(offsets, mix[t * here + slot]) * gains[:, cols]).astype(bf16)

    works = [head_part(g) for g in range(groups)] + [pool_part]
    for d in range(1, n_s):
        if works:
            works.pop(0)()
        hand_on(d)
    while works:
        works.pop(0)()

    lead_f, lead_b = spread(jnp.exp(run_f)), spread(jnp.exp(run_b))
    for g in range(groups):
        cols = slice(g * wide, (g + 1) * wide)
        reads = cut(1, g)
        mixed = inside[:, cols] + dot(reads, in_f[g]) * lead_f[:, cols]
        mixed = mixed + dot(reads, in_b[g]) * lead_b[:, cols]
        gate = proj[:, gate_at + g * wide : gate_at + (g + 1) * wide].astype(f32)
        inside[:, cols] = mixed * (gate * jax.nn.sigmoid(gate))
    gated = inside[...]
    high, low = split(gated * gated)
    mean = (dot(high, gather_m) + dot(low, gather_m)) * (1.0 / HEAD_DIM)
    scale = spread(lax.rsqrt(mean + EPSILON))
    mixer = (gated * scale * own(norm_gain, inner)).astype(bf16)

    for j in range(1, n_f):
        out_copy(j, lax.rem(f + n_f - j, n_f)).wait_recv()
    width = wo_inner.shape[1]
    for w in range(n_f):
        part[:, w * width : (w + 1) * width] = (
            dot(mixer, wo_i[w]) + dot(pooled[...], wo_p[w])
        ).astype(bf16)

    keep = rows // n_t

    def part_of(who):
        return pl.ds(pl.multiple_of(who * keep, keep), keep)

    def last_copy(i):
        to = lax.rem(t + i, n_t)
        return remote(
            part.at[part_of(to)], peer.at[i - 1], t_send.at[i - 1], t_recv.at[i - 1], "tp", to
        )

    for i in range(1, n_t):
        last_copy(i).start()
    for j in range(1, n_f):
        out_copy(j, f).wait_send()
    for g in range(groups):

        @pl.when(s + 1 < n_s)
        def _():
            chain_copy(True, g).wait_send()

        @pl.when(s >= 1)
        def _():
            chain_copy(False, g).wait_send()

    acc = part[part_of(t)].astype(f32)
    for i in range(1, n_t):
        last_copy(i).wait_recv()
        acc = acc + peer[i - 1].astype(f32)
    result[0] = acc.astype(bf16)
    for i in range(1, n_t):
        last_copy(i).wait_send()


def body(
    sizes, tokens, w_inner, w_gate, w_write, w_read, w_pool_in, w_step, conv_inner, conv_cross,
    rate_log, decay_extra, norm_gain, pool_mix, pool_gain, w_out_inner, w_out_pool,
):
    n_s, n_f, n_t = sizes
    tok = tokens[0]
    rows, half_d = tok.shape
    ks, inner = w_inner.shape
    cross = w_write.shape[1]
    pool = w_pool_in.shape[1]
    heads = inner // HEAD_DIM
    groups = cross // STATE
    stream = inner + 2 * cross
    total = stream + inner + pool
    hw = total // n_f // NH
    d = half_d * n_t

    step_w = w_step.reshape(d, 2 * heads * n_t)
    vmem = pl.BlockSpec(memory_space=pltpu.VMEM)
    dma = pltpu.SemaphoreType.DMA

    def shape(*dims, kind=bf16):
        return jax.ShapeDtypeStruct(dims, kind)

    moved = pl.pallas_call(
        functools.partial(project_kernel, sizes),
        out_shape=(
            shape(rows, total),
            shape(rows, 2 * heads, kind=f32),
            shape(RIM, stream),
            shape(RIM, stream),
            shape(rows, pool),
            shape(rows, pool),
            shape(n_f, *w_out_pool.shape),
        ),
        in_specs=[vmem] * 8,
        out_specs=(vmem,) * 7,
        scratch_shapes=[
            pltpu.VMEM((ks, total), bf16),
            pltpu.VMEM((NH, d, hw), bf16),
            pltpu.VMEM((n_f, n_t, rows, half_d), bf16),
            pltpu.VMEM((NH, n_f - 1, rows, hw), bf16),
            dma((NH, n_s)), dma((NH, n_s)), dma((NH, n_s)), dma((NH, n_s)),
            dma((n_f,)), dma((n_f,)), dma((n_f, n_t)), dma((n_f, n_t)),
            dma((NH, n_f - 1)), dma((NH, n_f - 1)), dma((4,)), dma((4,)),
            dma((n_f,)), dma((n_f,)),
        ],
        compiler_params=pltpu.CompilerParams(collective_id=0, has_side_effects=True),
    )(tok, w_inner, w_write, w_read, w_gate, w_pool_in, step_w, w_out_pool)

    result = pl.pallas_call(
        functools.partial(mixer_kernel, sizes),
        out_shape=shape(1, rows // n_t, d),
        in_specs=[vmem] * 15,
        scratch_shapes=[
            pltpu.VMEM((rows + 16, stream), f32),
            pltpu.VMEM((rows, stream), bf16),
            pltpu.VMEM((rows, inner), f32),
            pltpu.VMEM((n_f,) + w_out_inner.shape, bf16),
            pltpu.VMEM((groups, STATE, inner // groups), f32),
            pltpu.VMEM((groups, STATE, inner // groups), f32),
            pltpu.VMEM((groups, STATE, inner // groups), bf16),
            pltpu.VMEM((groups, STATE, inner // groups), bf16),
            pltpu.VMEM((groups, STATE, inner // groups), bf16),
            pltpu.VMEM((groups, STATE, inner // groups), bf16),
            pltpu.VMEM((rows, d), bf16),
            pltpu.VMEM((n_t - 1, rows // n_t, d), bf16),
            pltpu.VMEM((rows, pool), bf16),
            dma((n_f,)), dma((n_f,)), dma((groups,)), dma((groups,)),
            dma((groups,)), dma((groups,)), dma((n_t - 1,)), dma((n_t - 1,)),
        ],
        compiler_params=pltpu.CompilerParams(collective_id=1, has_side_effects=True),
    )(
        *moved,
        decay_extra[0].reshape(rows, 2 * heads),
        rate_log,
        conv_inner,
        conv_cross.reshape(CONV, -1),
        norm_gain[None],
        pool_mix,
        pool_gain[None],
        w_out_inner,
    )
    return result


def solution(mesh):
    sizes = tuple(mesh.shape[axis] for axis in ("sp", "fs", "tp"))
    return jax.shard_map(
        functools.partial(body, sizes),
        mesh=mesh,
        in_specs=(
            P("fs", "sp", "tp"),
            P("sp", "tp"),
            P("sp", "tp"),
            P("sp", "tp"),
            P("sp", "tp"),
            P("sp", "tp"),
            P(),
            P(),
            P(),
            P(),
            P("fs", "sp", None, "tp"),
            P(),
            P(),
            P(),
            P("tp", "fs"),
            P("tp", "fs"),
        ),
        out_specs=P("fs", ("sp", "tp"), None),
        check_vma=False,
    )
```
